32 devices in a mesh: grp: 2 (over y), ep: 8 (over z, x), tp: 2 (over core).
Axes of the slice: x: 2, y: 2, z: 4, core: 2. Of those that a mesh axis runs over, the one named last changes fastest.
Arguments:
- tokens: bfloat16 [4096, 2048], P(('grp', 'ep', 'tp')), parts along dimension 0, may hold values from -6 to 6
- expert_ids: int32 [4096, 4], P(('grp', 'ep', 'tp')), parts along dimension 0, may hold values from 0 to 15, all different within a row; in each aligned block of 128 rows (0 to 127, 128 to 255, ...) at most 48 rows name the same one
- gate_weights: float32 [4096, 4], P(('grp', 'ep', 'tp')), parts along dimension 0, may hold values from 0.1 to 1
- norm_gain: float32 [2048], replicated, may hold values from 0.1 to 1.9
- expert_gate: bfloat16 [16, 2048, 512], P(('ep', 'tp')), may hold values from -0.125 to 0.125
- expert_up: bfloat16 [16, 2048, 512], P(('ep', 'tp')), may hold values from -0.125 to 0.125
- expert_down: bfloat16 [16, 512, 2048], P(('ep', 'tp'))
- shared_gate: bfloat16 [2048, 512], P(None, 'tp'), may hold values from -0.125 to 0.125
- shared_up: bfloat16 [2048, 512], P(None, 'tp'), may hold values from -0.125 to 0.125
- shared_down: bfloat16 [512, 2048], P('tp')
- out_gain: float32 [2048], replicated, may hold values from 0.1 to 1.9
Outputs:
- layer_out: bfloat16 [4096, 2048], P(('grp', 'ep'), 'tp'), parts along dimension 0
The draws below stay inside these ranges and needn't reach their ends.
There are 2 independent parts, one for each index of `grp`. The reference program is written for one: setup_inputs(seed, part) draws one part's arguments, and reference() takes and returns one part's arrays. A program takes and returns all parts, laid end to end along the dimension named above; an argument that names none is the same for every part. Nothing has to cross between parts.
Inputs may be any that keep to these rules, and one draw needn't show every extreme that they name: `expert_ids`: each row names 4 different experts. Among the 128 rows of one device (aligned blocks of rows), no expert is named more than 48 times, and in every draw some expert is named exactly 48 times by some device.
All inputs are finite; a program needn't handle non-finite values.
Results may differ from the reference program's by a relative error of at most 0.0085.
Values may be sent and summed in bfloat16 or wider, within the bound.
A program may use at most 64 MiB of HBM per device.

```python
import math
import jax
import jax.numpy as jnp
import numpy as np
from jax import lax

D = 2048
FF = 512
SH = 512
TOPK = 4
TOK_DEV = 128
EXPERTS = 16
CAP = 48
TOKENS = 2048
N_EP = 8
N_TP = 2


def rising_columns(key, shape, fan_in):
    base = jax.random.normal(key, shape, jnp.float32)
    columns = shape[-1]
    rise = 10.0 ** (jnp.arange(columns, dtype=jnp.float32) / (columns - 1))
    return base * rise * fan_in ** (-0.5)


def draw_expert_down(key, part):
    return rising_columns(jax.random.fold_in(key, 11), (EXPERTS, FF, D), FF).astype(jnp.bfloat16)


def draw_shared_down(key, part):
    return rising_columns(jax.random.fold_in(key, 23), (SH, D), SH).astype(jnp.bfloat16)


def block_scale(rng, shape, pieces, least, top_value):
    def one(position, shards_of):
        steps = jax.random.uniform(jax.random.fold_in(jax.random.fold_in(rng, 6), position), (shards_of,), jnp.float32, least / len(pieces), top_value / len(pieces))
        return jnp.repeat(jnp.exp(steps), shape[position] // shards_of).reshape((-1,) + (1,) * (len(shape) - position - 1))

    loudness = one(*pieces[0])
    for cut in pieces[1:]:
        loudness = loudness * one(*cut)
    return loudness


def deal_out(rng, own, number, rows, amount, top, most, skew):
    sequence = jax.random.permutation(rng, amount)
    packed, usual = shares(amount, rows * top, most, skew, True), shares(amount, rows * top, most, skew, False)
    places = jnp.arange(amount)

    def named(tallies, offset_by):
        used = int((tallies > 0).sum())
        fixed = max(1, used // 4)
        moved = fixed + (places - fixed + offset_by * (used - fixed)) % max(1, amount - fixed)
        return jnp.zeros((amount,), jnp.int32).at[sequence[jnp.where(places < fixed, places, moved)]].set(jnp.asarray(tallies, jnp.int32))

    tallies = jnp.where(number % 4 == 0, named(packed, number // 4), named(usual, number - number // 4 - 1))
    mixed = jax.random.permutation(jax.random.fold_in(own, 3), amount)
    donor, sink = mixed[0:amount // 2 * 2:2], mixed[1:amount // 2 * 2:2]
    room = jnp.minimum(tallies[donor] - 1, most - tallies[sink]) // 2
    room = jnp.where((donor == sequence[0]) | (sink == sequence[0]) | (tallies[sink] == 0), 0, jnp.maximum(room, 0))
    moved = jax.random.randint(jax.random.fold_in(own, 4), (amount // 2,), 0, 1 << 20) % (room + 1)
    tallies = tallies.at[donor].add(-moved).at[sink].add(moved)
    labels = jnp.searchsorted(jnp.cumsum(tallies), jnp.arange(rows * top), side="right").astype(jnp.int32)
    table = labels.reshape(top, rows).T
    table = table[jax.random.permutation(jax.random.fold_in(own, 1), rows)]
    offset_by = jax.random.randint(jax.random.fold_in(own, 2), (rows, 1), 0, top)
    return jnp.take_along_axis(table, (jnp.arange(top)[None, :] + offset_by) % top, axis=1)


def shares(amount, total, reach, lean, full):
    loads = [(1 << 20) // math.isqrt(standing ** lean) + 1 for standing in range(1, amount + 1)]
    largest = reach if full else min(reach, max(-(-total // amount), total * loads[0] // sum(loads)))
    least = 1 if total - largest >= amount - 1 else 0
    given, spare = [largest] + [least] * (amount - 1), total - largest - least * (amount - 1)
    while spare > 0:
        movable = [i for i in range(1, amount) if given[i] < largest] or [i for i in range(1, amount) if given[i] < reach]
        whole, remaining = sum([loads[i] for i in movable]), spare
        for i in movable:
            extra = min(reach - given[i], max(1, remaining * loads[i] // whole), spare)
            given[i] = given[i] + extra
            spare = spare - extra
    return np.array(given)


def normal_values(rng, dims, deviation, bound, pieces=(), kind=jnp.bfloat16):
    drawn = deviation * jax.random.normal(rng, dims, jnp.float32)
    if pieces:
        drawn = drawn * block_scale(rng, dims, pieces, -0.22, 0.18)
    return jnp.clip(drawn, -bound, bound).astype(kind)


def setup_inputs(seed: int = 0, part: int = 0) -> dict:
    arg_keys = jax.random.split(jax.random.key(seed), 12)
    part_keys = jax.random.split(jax.random.fold_in(arg_keys[11], part), 12)
    tokens = normal_values(part_keys[0], (TOKENS, D), 1.0, 6.0, ((0, 16),))
    expert_ids_keys = jax.random.split(jax.random.fold_in(part_keys[1], 1), TOKENS // TOK_DEV)
    expert_ids_turns = jax.random.permutation(jax.random.fold_in(part_keys[1], 3), TOKENS // TOK_DEV)
    expert_ids = jax.vmap(lambda own, number: deal_out(jax.random.fold_in(part_keys[1], 2), own, number, TOK_DEV, EXPERTS, TOPK, CAP, 2))(expert_ids_keys, expert_ids_turns).reshape((TOKENS, TOPK))
    gate_weights = jnp.clip(jnp.exp(math.log(1.0) - 2.3025851 * jax.random.uniform(part_keys[2], (TOKENS, TOPK), jnp.float32) ** block_scale(part_keys[2], (TOKENS, TOPK), ((0, 16),), -0.2, 0.2)), 0.1, 1.0)
    norm_gain = jnp.clip(1.0 + 0.18 * jax.random.normal(arg_keys[3], (D,), jnp.float32), 0.1, 1.9)
    expert_gate = normal_values(arg_keys[4], (EXPERTS, D, FF), D ** -0.5, 0.125, ((0, 16),))
    expert_up = normal_values(arg_keys[5], (EXPERTS, D, FF), D ** -0.5, 0.125, ((0, 16),))
    expert_down = draw_expert_down(jax.random.fold_in(arg_keys[11], 71), part)
    shared_gate = normal_values(arg_keys[7], (D, SH), D ** -0.5, 0.125, ((1, 2),))
    shared_up = normal_values(arg_keys[8], (D, SH), D ** -0.5, 0.125, ((1, 2),))
    shared_down = draw_shared_down(jax.random.fold_in(arg_keys[11], 71), part)
    out_gain = jnp.clip(1.0 + 0.18 * jax.random.normal(arg_keys[10], (D,), jnp.float32), 0.1, 1.9)
    return {"tokens": tokens, "expert_ids": expert_ids, "gate_weights": gate_weights, "norm_gain": norm_gain, "expert_gate": expert_gate, "expert_up": expert_up, "expert_down": expert_down, "shared_gate": shared_gate, "shared_up": shared_up, "shared_down": shared_down, "out_gain": out_gain}


def reference(tokens, expert_ids, gate_weights, norm_gain, expert_gate, expert_up, expert_down, shared_gate, shared_up, shared_down, out_gain):
    values = tokens.astype(jnp.float32)
    scale = lax.rsqrt(lax.optimization_barrier(jnp.mean(values * values, axis=1, keepdims=True)) + 1e-06)
    normed = (values * scale * norm_gain).astype(jnp.bfloat16)
    flat_ids = expert_ids.reshape(-1)
    flat_gates = gate_weights.reshape(-1)
    copy_count = TOKENS * TOPK
    most_rows = N_EP * N_TP * CAP

    def one_expert(total, inputs):
        w_gate, w_up, w_down, expert_index = inputs
        positions = jnp.nonzero(flat_ids == expert_index, size=most_rows, fill_value=copy_count)[0].astype(jnp.int32)
        valid = positions < copy_count
        clipped = jnp.minimum(positions, copy_count - 1)
        token_index = clipped // TOPK
        weight = jnp.where(valid, flat_gates[clipped], 0.0)
        rows = normed[token_index]
        gate = jnp.dot(rows, w_gate, preferred_element_type=jnp.float32)
        upper = jnp.dot(rows, w_up, preferred_element_type=jnp.float32)
        hidden = (jax.nn.silu(gate) * upper).astype(jnp.bfloat16)
        result = jnp.dot(hidden, w_down, preferred_element_type=jnp.float32).astype(jnp.bfloat16)
        total = total.at[token_index].add(result.astype(jnp.float32) * weight[:, None])
        return (total, None)
    routed, _ = lax.scan(one_expert, jnp.zeros((TOKENS, D), jnp.float32), (expert_gate, expert_up, expert_down, jnp.arange(EXPERTS, dtype=jnp.int32)))
    shared_hidden = (jax.nn.silu(jnp.dot(normed, shared_gate, preferred_element_type=jnp.float32)) * jnp.dot(normed, shared_up, preferred_element_type=jnp.float32)).astype(jnp.bfloat16)
    shared_out = jnp.dot(shared_hidden, shared_down, preferred_element_type=jnp.float32)
    mixed = (routed + shared_out).astype(jnp.bfloat16).astype(jnp.float32)
    final_scale = lax.rsqrt(lax.optimization_barrier(jnp.mean(mixed * mixed, axis=1, keepdims=True)) + 1e-06)
    return (mixed * final_scale * out_gain).astype(jnp.bfloat16)
```

```python
import functools

import jax
import jax.numpy as jnp
from jax import lax
from jax.experimental import pallas as pl
from jax.experimental.pallas import tpu as pltpu
from jax.sharding import PartitionSpec as P

MESH = pl.DeviceIdType.MESH
F32 = jnp.float32
BF16 = jnp.bfloat16


def ring_kernel(
    n,
    ids_ref,
    gates_ref,
    tok_ref,
    gain_ref,
    out_gain_ref,
    eg_hbm,
    eu_hbm,
    ed_hbm,
    sg_hbm,
    su_hbm,
    sd_hbm,
    out_ref,
    own_x,
    own_w,
    rx,
    wrx,
    wg,
    wu,
    wd_mine,
    wd_other,
    sg,
    su,
    sd_mine,
    sd_other,
    kept,
    psend,
    prx,
    home,
    home_send,
    home_rx,
    rs_send,
    rs_rx,
    sq_send,
    sq_rx,
    load_sem,
    ag_ssem,
    ag_rsem,
    w_ssem,
    w_rsem,
    pag_ssem,
    pag_rsem,
    pw_ssem,
    pw_rsem,
    ox_ssem,
    ox_rsem,
    p_ssem,
    p_rsem,
    h_ssem,
    h_rsem,
    rs_ssem,
    rs_rsem,
    sq_ssem,
    sq_rsem,
):
    slots = n - 1
    rows, width = tok_ref.shape
    half = rows // 2
    cols = width // 2
    topk = ids_ref.shape[1]
    experts = own_w.shape[1]
    turn = n // 2
    ep = lax.axis_index("ep")
    c = lax.axis_index("tp")
    oc = 1 - c
    x = ep % 2
    z = ep // 2
    pos = z * (1 - x) + (n - 1 - z) * x

    def at(p):
        q = p // turn
        return 2 * p * (1 - q) + (2 * (n - 1 - p) + 1) * q

    toward = (at((pos + 1) % n), at((pos + n - 1) % n))
    mine = ep * 2 + c

    barrier = pltpu.get_barrier_semaphore()
    for e in toward:
        pl.semaphore_signal(barrier, inc=1, device_id={"ep": e, "tp": c}, device_id_type=MESH)
    pl.semaphore_signal(barrier, inc=1, device_id={"ep": ep, "tp": oc}, device_id_type=MESH)

    lo, hi = pl.ds(pl.multiple_of(c * cols, cols), cols), pl.ds(pl.multiple_of(oc * cols, cols), cols)
    loads = [
        (eg_hbm.at[0], wg),
        (eu_hbm.at[0], wu),
        (ed_hbm.at[0, :, hi], wd_other),
        (ed_hbm.at[0, :, lo], wd_mine),
        (sg_hbm, sg),
        (su_hbm, su),
        (sd_hbm.at[:, hi], sd_other),
        (sd_hbm.at[:, lo], sd_mine),
    ]
    loads = [pltpu.make_async_copy(s, d, load_sem.at[i]) for i, (s, d) in enumerate(loads)]
    for load in loads:
        load.start()

    values = tok_ref[...].astype(F32)
    scale = lax.rsqrt(jnp.mean(values * values, axis=1, keepdims=True) + 1e-06)
    own_x[c] = (values * scale * gain_ref[...]).astype(BF16)
    lane = lax.broadcasted_iota(jnp.int32, (rows, 128), 1)
    dense = jnp.zeros((rows, 128), F32)
    for k in range(topk):
        dense += jnp.where(ids_ref[:, k : k + 1] == lane, gates_ref[:, k : k + 1], 0.0)
    own_w[c] = dense.T[:experts]

    pl.semaphore_wait(barrier, 3)

    def remote(src, dst, ssem, rsem, e, core):
        return pltpu.make_async_remote_copy(
            src_ref=src,
            dst_ref=dst,
            send_sem=ssem,
            recv_sem=rsem,
            device_id={"ep": e, "tp": core},
            device_id_type=MESH,
        )

    def ag(s, d, src):
        return remote(src, rx.at[s, d, c], ag_ssem.at[s, d], ag_rsem.at[s, d], toward[d], c)

    def agw(i, d, src):
        return remote(src, wrx.at[i, d, c], w_ssem.at[i, d], w_rsem.at[i, d], toward[d], c)

    def pag(s, d, core):
        return remote(
            rx.at[s, d, core], rx.at[s, d, core], pag_ssem.at[s, d], pag_rsem.at[s, d], ep, oc
        )

    def pagw(i, d, core):
        return remote(
            wrx.at[i, d, core], wrx.at[i, d, core], pw_ssem.at[i, d], pw_rsem.at[i, d], ep, oc
        )

    def own_half(h):
        return own_x.at[c, pl.ds(h * half, half)]

    for d in range(2):
        agw(0, d, own_w.at[c]).start()
        ag(0, d, own_half(d)).start()
    home_copies = (
        lambda core: remote(own_x.at[core], own_x.at[core], ox_ssem.at[0], ox_rsem.at[0], ep, oc),
        lambda core: remote(own_w.at[core], own_w.at[core], ox_ssem.at[1], ox_rsem.at[1], ep, oc),
    )
    for copy in home_copies:
        copy(c).start()
    for d in range(2):
        ag(1, d, own_half(1 - d)).start()

    def silu_mul(g, u):
        return (g / (1.0 + jnp.exp(-g)) * u).astype(BF16)

    def dot(a, b):
        return jnp.dot(a, b, preferred_element_type=F32)

    def column(row, offset, count):
        r = lax.broadcasted_iota(jnp.int32, (count, rows), 0) + offset
        q = lax.broadcasted_iota(jnp.int32, (count, rows), 1)
        return jnp.sum(jnp.where(r == q, row, 0.0), axis=1, keepdims=True)

    for load in loads:
        load.wait()
    for copy in home_copies:
        copy(oc).wait_recv()

    xs = own_x[...].reshape(2 * rows, width)
    hidden = silu_mul(dot(xs, wg[...]), dot(xs, wu[...]))
    shared = silu_mul(dot(xs, sg[...]), dot(xs, su[...]))
    weight = jnp.concatenate(
        [column(own_w[k, pl.ds(mine, 1), :], 0, rows) for k in range(2)], axis=0
    )
    home_send[...] = dot(hidden, wd_other[...]) * weight + dot(shared, sd_other[...])
    home[...] = dot(hidden, wd_mine[...]) * weight + dot(shared, sd_mine[...])
    home_copy = remote(home_send, home_rx, h_ssem.at[0], h_rsem.at[0], ep, oc)
    home_copy.start()

    def partner(s):
        return remote(psend.at[s], prx.at[s], p_ssem.at[s], p_rsem.at[s], ep, oc)

    def step(s, _):
        i = s // 2
        even = s % 2 == 0
        for d in range(2):
            ag(s, d, rx.at[s, d, c]).wait_recv()

            @pl.when(s + 2 < slots)
            def _():
                ag(s + 2, d, rx.at[s, d, c]).start()

            pag(s, d, c).start()

            @pl.when(even)
            def _():
                agw(i, d, wrx.at[i, d, c]).wait_recv()

                @pl.when(s + 2 < slots)
                def _():
                    agw(i + 1, d, wrx.at[i, d, c]).start()

                pagw(i, d, c).start()

        for d in range(2):
            pag(s, d, oc).wait_recv()

            @pl.when(even)
            def _():
                pagw(i, d, oc).wait_recv()

        weight = jnp.concatenate(
            [
                column(
                    wrx[i, d, k, pl.ds(mine, 1), :],
                    (s % 2) * half if d == 0 else (1 - s % 2) * half,
                    half,
                )
                for d in range(2)
                for k in range(2)
            ],
            axis=0,
        )
        xs = rx[s].reshape(2 * rows, width)
        hidden = silu_mul(dot(xs, wg[...]), dot(xs, wu[...]))
        psend[s] = (dot(hidden, wd_other[...]) * weight).astype(BF16)
        kept[s] = dot(hidden, wd_mine[...]) * weight
        partner(s).start()
        return 0

    def back(s, d):
        return remote(
            rs_send.at[s, d], rs_rx.at[s, d], rs_ssem.at[s, d], rs_rsem.at[s, d], toward[1 - d], c
        )

    def give(s, further):
        partner(s).wait_recv()
        for d in range(2):
            part = pl.ds(d * rows, rows)
            total = kept[s, part, :] + prx[s, part, :].astype(F32)
            if further:
                back(s + 2, d).wait_recv()
                total += rs_rx[s + 2, d].astype(F32)
            rs_send[s, d] = total.astype(BF16)
            back(s, d).start()

    lax.fori_loop(0, slots - 1, step, 0)
    give(slots - 2, False)
    lax.fori_loop(slots - 1, slots, step, 0)
    give(slots - 1, False)
    for s in [t for k in range(slots - 4, -1, -2) for t in (k, k + 1)] + [0]:
        give(s, True)

    home_copy.wait_recv()
    mixed = []
    for s in range(2):
        for d in range(2):
            back(s, d).wait_recv()
    for k in range(2):
        for h in range(2):
            part = pl.ds(k * rows + h * half, half)
            got = pl.ds(k * half, half)
            total = home[part, :] + home_rx[part, :]
            total += rs_rx[h, 0, got, :].astype(F32) + rs_rx[1 - h, 1, got, :].astype(F32)
            rounded = total.astype(BF16).astype(F32)
            home[part, :] = rounded
            sq = jnp.sum(rounded * rounded, axis=1, keepdims=True)
            sq_send[part, :] = jnp.broadcast_to(sq, (half, 128))
    sq_copy = remote(sq_send, sq_rx, sq_ssem.at[0], sq_rsem.at[0], ep, oc)
    sq_copy.start()
    sq_copy.wait_recv()
    total = (sq_send[...] + sq_rx[...])[:, :1]
    final = lax.rsqrt(total / width + 1e-06)
    out_ref[...] = (home[...] * final * out_gain_ref[c]).astype(BF16)

    for d in range(2):
        for s in range(slots):
            ag(s, d, rx.at[s, d, c]).wait_send()
            pag(s, d, c).wait_send()
            back(s, d).wait_send()
        for i in range(turn):
            agw(i, d, wrx.at[i, d, c]).wait_send()
            pagw(i, d, c).wait_send()
    for s in range(slots):
        partner(s).wait_send()
    for copy in home_copies:
        copy(c).wait_send()
    home_copy.wait_send()
    sq_copy.wait_send()


def ring_local(
    n,
    tokens,
    expert_ids,
    gate_weights,
    norm_gain,
    expert_gate,
    expert_up,
    expert_down,
    shared_gate,
    shared_up,
    shared_down,
    out_gain,
):
    rows, width = tokens.shape
    ff = expert_gate.shape[2]
    sh = shared_gate.shape[1]
    cols = width // 2
    slots, turn, half = n - 1, n // 2, rows // 2
    experts = 2 * n * expert_gate.shape[0]
    dma = pltpu.SemaphoreType.DMA
    vmem = pl.BlockSpec(memory_space=pltpu.VMEM)
    hbm = pl.BlockSpec(memory_space=pl.ANY)
    return pl.pallas_call(
        functools.partial(ring_kernel, n),
        out_shape=jax.ShapeDtypeStruct((2 * rows, cols), BF16),
        in_specs=[vmem] * 5 + [hbm] * 6,
        out_specs=vmem,
        scratch_shapes=[
            pltpu.VMEM((2, rows, width), BF16),
            pltpu.VMEM((2, experts, rows), F32),
            pltpu.VMEM((slots, 2, 2, half, width), BF16),
            pltpu.VMEM((turn, 2, 2, experts, rows), F32),
            pltpu.VMEM((width, ff), BF16),
            pltpu.VMEM((width, ff), BF16),
            pltpu.VMEM((ff, cols), BF16),
            pltpu.VMEM((ff, cols), BF16),
            pltpu.VMEM((width, sh), BF16),
            pltpu.VMEM((width, sh), BF16),
            pltpu.VMEM((sh, cols), BF16),
            pltpu.VMEM((sh, cols), BF16),
            pltpu.VMEM((slots, 2 * rows, cols), F32),
            pltpu.VMEM((slots, 2 * rows, cols), BF16),
            pltpu.VMEM((slots, 2 * rows, cols), BF16),
            pltpu.VMEM((2 * rows, cols), F32),
            pltpu.VMEM((2 * rows, cols), F32),
            pltpu.VMEM((2 * rows, cols), F32),
            pltpu.VMEM((slots, 2, rows, cols), BF16),
            pltpu.VMEM((slots, 2, rows, cols), BF16),
            pltpu.VMEM((2 * rows, 128), F32),
            pltpu.VMEM((2 * rows, 128), F32),
            dma((8,)),
            dma((slots, 2)),
            dma((slots, 2)),
            dma((turn, 2)),
            dma((turn, 2)),
            dma((slots, 2)),
            dma((slots, 2)),
            dma((turn, 2)),
            dma((turn, 2)),
            dma((2,)),
            dma((2,)),
            dma((slots,)),
            dma((slots,)),
            dma((1,)),
            dma((1,)),
            dma((slots, 2)),
            dma((slots, 2)),
            dma((1,)),
            dma((1,)),
        ],
        compiler_params=pltpu.CompilerParams(
            collective_id=0, has_side_effects=True, vmem_limit_bytes=60 * 1024 * 1024
        ),
    )(
        expert_ids,
        gate_weights,
        tokens,
        norm_gain.reshape(1, width),
        out_gain.reshape(2, 1, cols),
        expert_gate,
        expert_up,
        expert_down,
        shared_gate,
        shared_up,
        shared_down,
    )


TOPK = 4


def expert_work(received, expert_gate, expert_up, expert_down):
    gate = jnp.einsum("slcd,ldf->slcf", received, expert_gate, preferred_element_type=jnp.float32)
    upper = jnp.einsum("slcd,ldf->slcf", received, expert_up, preferred_element_type=jnp.float32)
    hidden = (jax.nn.silu(gate) * upper).astype(jnp.bfloat16)
    return jnp.einsum(
        "slcf,lfd->slcd", hidden, expert_down, preferred_element_type=jnp.float32
    ).astype(jnp.bfloat16)


def local(
    tokens,
    expert_ids,
    gate_weights,
    norm_gain,
    expert_gate,
    expert_up,
    expert_down,
    shared_gate,
    shared_up,
    shared_down,
    out_gain,
):
    local_rows = tokens.shape[0]
    width = tokens.shape[1]
    ep_count = lax.axis_size("ep")
    tp_count = lax.axis_size("tp")
    device_count = ep_count * tp_count
    local_experts = expert_gate.shape[0]
    expert_count = device_count * local_experts
    capacity = 3 * local_rows * TOPK // (2 * expert_count)
    values = tokens.astype(jnp.float32)
    scale = lax.rsqrt(jnp.mean(values * values, axis=1, keepdims=True) + 1e-06)
    normed = (values * scale * norm_gain).astype(jnp.bfloat16)
    flat_ids = expert_ids.reshape(-1)
    one_hot = (flat_ids[:, None] == jnp.arange(expert_count, dtype=jnp.int32)[None, :]).astype(
        jnp.int32
    )
    earlier = jnp.cumsum(one_hot, axis=0) - one_hot
    slot_index = jnp.sum(earlier * one_hot, axis=1)
    target = flat_ids * capacity + slot_index
    copy_rows = normed[jnp.arange(local_rows * TOPK, dtype=jnp.int32) // TOPK]
    outgoing = jnp.zeros((expert_count * capacity, width), jnp.bfloat16).at[target].set(copy_rows)
    sending = outgoing.reshape(device_count, local_experts * capacity, width)
    received = lax.all_to_all(sending, ("ep", "tp"), split_axis=0, concat_axis=0, tiled=True)
    received = received.reshape(device_count, local_experts, capacity, width)
    results = expert_work(received, expert_gate, expert_up, expert_down)
    results = results.reshape(device_count, local_experts * capacity, width)
    returned = lax.all_to_all(results, ("ep", "tp"), split_axis=0, concat_axis=0, tiled=True)
    returned = returned.reshape(expert_count * capacity, width)
    picked = returned[target].astype(jnp.float32).reshape(local_rows, TOPK, width)
    routed = jnp.sum(picked * gate_weights[:, :, None], axis=1)
    piece = lax.all_gather(normed, "tp", axis=0, tiled=True)
    gate = jnp.dot(piece, shared_gate, preferred_element_type=jnp.float32)
    upper = jnp.dot(piece, shared_up, preferred_element_type=jnp.float32)
    shared_hidden = (jax.nn.silu(gate) * upper).astype(jnp.bfloat16)
    shared_out = lax.psum_scatter(
        jnp.dot(shared_hidden, shared_down, preferred_element_type=jnp.float32),
        "tp",
        scatter_dimension=0,
        tiled=True,
    )
    mixed = (routed + shared_out).astype(jnp.bfloat16)
    mixed_values = mixed.astype(jnp.float32)
    final_scale = lax.rsqrt(jnp.mean(mixed_values * mixed_values, axis=1, keepdims=True) + 1e-06)
    normalized = (mixed_values * final_scale * out_gain).astype(jnp.bfloat16)
    return lax.all_to_all(normalized, "tp", split_axis=1, concat_axis=0, tiled=True)


def solution(mesh):
    in_specs = (
        P(("grp", "ep", "tp"), None),
        P(("grp", "ep", "tp"), None),
        P(("grp", "ep", "tp"), None),
        P(),
        P(("ep", "tp"), None, None),
        P(("ep", "tp"), None, None),
        P(("ep", "tp"), None, None),
        P(None, "tp"),
        P(None, "tp"),
        P("tp", None),
        P(),
    )
    out_specs = P(("grp", "ep"), "tp")
    n, tp = mesh.shape["ep"], mesh.shape["tp"]

    def run(*args):
        tokens, expert_gate = args[0], args[4]
        rows = tokens.shape[0] // mesh.size
        experts = expert_gate.shape[0]
        dense = experts == n * tp and experts <= 8 * args[1].shape[1]
        dense = dense and tp == 2 and n % 2 == 0 and n >= 4 and rows == 128
        body = functools.partial(ring_local, n) if dense else local
        return jax.shard_map(
            body, mesh=mesh, in_specs=in_specs, out_specs=out_specs, check_vma=False
        )(*args)

    return run
```

```python
import functools

import jax
import jax.numpy as jnp
from jax import lax
from jax.experimental import pallas as pl
from jax.experimental.pallas import tpu as pltpu
from jax.sharding import PartitionSpec as P

MESH = pl.DeviceIdType.MESH
PARTS = 2
F32 = jnp.float32
BF16 = jnp.bfloat16


def ring_kernel(
    n,
    ids_ref,
    gates_ref,
    tok_ref,
    gain_ref,
    eg_hbm,
    eu_hbm,
    ed_hbm,
    sg_hbm,
    su_hbm,
    sd_hbm,
    out_ref,
    sq_ref,
    own_x,
    own_w,
    rx,
    wrx,
    wg,
    wu,
    wd_mine,
    wd_other,
    sg,
    su,
    sd_mine,
    sd_other,
    kept,
    psend,
    prx,
    home,
    home_send,
    home_rx,
    rs_send,
    rs_rx,
    sq_send,
    sq_rx,
    load_sem,
    ag_ssem,
    ag_rsem,
    w_ssem,
    w_rsem,
    pag_ssem,
    pag_rsem,
    pw_ssem,
    pw_rsem,
    ox_ssem,
    ox_rsem,
    p_ssem,
    p_rsem,
    h_ssem,
    h_rsem,
    rs_ssem,
    rs_rsem,
    sq_ssem,
    sq_rsem,
):
    per = 2 * PARTS
    slots = (n - 1) * PARTS
    rows, width = tok_ref.shape
    chunk = rows // per
    cols = width // 2
    topk = ids_ref.shape[0]
    experts = own_w.shape[1]
    turn = n // 2
    ep = lax.axis_index("ep")
    c = lax.axis_index("tp")
    oc = 1 - c
    x = ep % 2
    z = ep // 2
    pos = z * (1 - x) + (n - 1 - z) * x

    def at(p):
        q = p // turn
        return 2 * p * (1 - q) + (2 * (n - 1 - p) + 1) * q

    toward = (at((pos + 1) % n), at((pos + n - 1) % n))
    mine = ep * 2 + c

    barrier = pltpu.get_barrier_semaphore()
    for e in toward:
        pl.semaphore_signal(barrier, inc=1, device_id={"ep": e, "tp": c}, device_id_type=MESH)
    pl.semaphore_signal(barrier, inc=1, device_id={"ep": ep, "tp": oc}, device_id_type=MESH)

    lo, hi = pl.ds(pl.multiple_of(c * cols, cols), cols), pl.ds(pl.multiple_of(oc * cols, cols), cols)
    loads = [
        (eg_hbm.at[0], wg),
        (eu_hbm.at[0], wu),
        (ed_hbm.at[0, :, hi], wd_other),
        (ed_hbm.at[0, :, lo], wd_mine),
        (sg_hbm, sg),
        (su_hbm, su),
        (sd_hbm.at[:, hi], sd_other),
        (sd_hbm.at[:, lo], sd_mine),
    ]
    loads = [pltpu.make_async_copy(s, d, load_sem.at[i]) for i, (s, d) in enumerate(loads)]
    for load in loads:
        load.start()

    values = tok_ref[...].astype(F32)
    scale = lax.rsqrt(jnp.mean(values * values, axis=1, keepdims=True) + 1e-06)
    own_x[c] = (values * scale * gain_ref[...]).astype(BF16)
    expert = lax.broadcasted_iota(jnp.int32, (experts, rows), 0)
    dense = jnp.zeros((experts, rows), F32)
    for k in range(topk):
        dense += jnp.where(ids_ref[k : k + 1, :] == expert, gates_ref[k : k + 1, :], 0.0)
    own_w[c] = dense

    pl.semaphore_wait(barrier, 3)

    def remote(src, dst, ssem, rsem, e, core):
        return pltpu.make_async_remote_copy(
            src_ref=src,
            dst_ref=dst,
            send_sem=ssem,
            recv_sem=rsem,
            device_id={"ep": e, "tp": core},
            device_id_type=MESH,
        )

    def ag(s, d, src):
        return remote(src, rx.at[s, d, c], ag_ssem.at[s, d], ag_rsem.at[s, d], toward[d], c)

    def agw(i, d, src):
        return remote(src, wrx.at[i, d, c], w_ssem.at[i, d], w_rsem.at[i, d], toward[d], c)

    def pag(s, d, core):
        return remote(
            rx.at[s, d, core], rx.at[s, d, core], pag_ssem.at[s, d], pag_rsem.at[s, d], ep, oc
        )

    def pagw(i, d, core):
        return remote(
            wrx.at[i, d, core], wrx.at[i, d, core], pw_ssem.at[i, d], pw_rsem.at[i, d], ep, oc
        )

    def place(s, d):
        return (s + d * PARTS) % per

    def own_chunk(s, d):
        return own_x.at[c, pl.ds(place(s, d) * chunk, chunk)]

    for d in range(2):
        agw(0, d, own_w.at[c]).start()
        ag(0, d, own_chunk(0, d)).start()
    home_copies = (
        lambda core: remote(own_x.at[core], own_x.at[core], ox_ssem.at[0], ox_rsem.at[0], ep, oc),
        lambda core: remote(own_w.at[core], own_w.at[core], ox_ssem.at[1], ox_rsem.at[1], ep, oc),
    )
    for copy in home_copies:
        copy(c).start()
    for s in range(1, per):
        for d in range(2):
            ag(s, d, own_chunk(s, d)).start()

    def silu_mul(g, u):
        return (g / (1.0 + jnp.exp(-g)) * u).astype(BF16)

    def dot(a, b):
        return jnp.dot(a, b, preferred_element_type=F32)

    def column(row, offset, count):
        r = lax.broadcasted_iota(jnp.int32, (count, rows), 0) + offset
        q = lax.broadcasted_iota(jnp.int32, (count, rows), 1)
        return jnp.sum(jnp.where(r == q, row, 0.0), axis=1, keepdims=True)

    for load in loads:
        load.wait()
    for copy in home_copies:
        copy(oc).wait_recv()

    xs = own_x[...].reshape(2 * rows, width)
    hidden = silu_mul(dot(xs, wg[...]), dot(xs, wu[...]))
    shared = silu_mul(dot(xs, sg[...]), dot(xs, su[...]))
    weight = jnp.concatenate(
        [column(own_w[k, pl.ds(mine, 1), :], 0, rows) for k in range(2)], axis=0
    )
    home_send[...] = dot(hidden, wd_other[...]) * weight + dot(shared, sd_other[...])
    home[...] = dot(hidden, wd_mine[...]) * weight + dot(shared, sd_mine[...])
    home_copy = remote(home_send, home_rx, h_ssem.at[0], h_rsem.at[0], ep, oc)
    home_copy.start()

    def partner(s):
        return remote(psend.at[s], prx.at[s], p_ssem.at[s], p_rsem.at[s], ep, oc)

    def step(s, _):
        i = s // per
        first = s % per == 0
        for d in range(2):
            ag(s, d, rx.at[s, d, c]).wait_recv()

            @pl.when(s + per < slots)
            def _():
                ag(s + per, d, rx.at[s, d, c]).start()

            pag(s, d, c).start()

            @pl.when(first)
            def _():
                agw(i, d, wrx.at[i, d, c]).wait_recv()

                @pl.when(s + per < slots)
                def _():
                    agw(i + 1, d, wrx.at[i, d, c]).start()

                pagw(i, d, c).start()

        for d in range(2):
            pag(s, d, oc).wait_recv()

            @pl.when(first)
            def _():
                pagw(i, d, oc).wait_recv()

        weight = jnp.concatenate(
            [
                column(
                    wrx[i, d, k, pl.ds(mine, 1), :],
                    place(s, d) * chunk,
                    chunk,
                )
                for d in range(2)
                for k in range(2)
            ],
            axis=0,
        )
        xs = rx[s].reshape(4 * chunk, width)
        hidden = silu_mul(dot(xs, wg[...]), dot(xs, wu[...]))
        psend[s] = (dot(hidden, wd_other[...]) * weight).astype(BF16)
        kept[s] = dot(hidden, wd_mine[...]) * weight
        partner(s).start()
        return 0

    def back(s, d):
        return remote(
            rs_send.at[s, d], rs_rx.at[s, d], rs_ssem.at[s, d], rs_rsem.at[s, d], toward[1 - d], c
        )

    def give(s, further):
        partner(s).wait_recv()
        for d in range(2):
            part = pl.ds(d * 2 * chunk, 2 * chunk)
            total = kept[s, part, :] + prx[s, part, :].astype(F32)
            if further:
                back(s + per, d).wait_recv()
                total += rs_rx[s + per, d].astype(F32)
            rs_send[s, d] = total.astype(BF16)
            back(s, d).start()

    for s in range(slots - per, slots):
        lax.fori_loop(s if s > slots - per else 0, s + 1, step, 0)
        give(s, False)
    home_copy.wait_recv()
    home[...] += home_rx[...]
    order = [s for k in range(slots - 2 * per, -1, -per) for s in range(k, k + per)]
    for s in order + list(range(slots % per)):
        give(s, True)

    for s in [*range(PARTS, per), *range(PARTS)]:
        for d in range(2):
            back(s, d).wait_recv()
            for k in range(2):
                part = pl.ds(k * rows + place(s, d) * chunk, chunk)
                total = home[part, :] + rs_rx[s, d, pl.ds(k * chunk, chunk), :].astype(F32)
                if s >= PARTS:
                    home[part, :] = total
                else:
                    mixed = total.astype(BF16)
                    out_ref[part, :] = mixed
                    mixed = mixed.astype(F32)
                    sq = jnp.sum(mixed * mixed, axis=1, keepdims=True)
                    sq_send[part, :] = jnp.broadcast_to(sq, (chunk, 128))
    sq_copy = remote(sq_send, sq_rx, sq_ssem.at[0], sq_rsem.at[0], ep, oc)
    sq_copy.start()
    sq_copy.wait_recv()
    sq_ref[...] = sq_send[...] + sq_rx[...]

    for d in range(2):
        for s in range(slots):
            ag(s, d, rx.at[s, d, c]).wait_send()
            pag(s, d, c).wait_send()
            back(s, d).wait_send()
        for i in range(turn):
            agw(i, d, wrx.at[i, d, c]).wait_send()
            pagw(i, d, c).wait_send()
    for s in range(slots):
        partner(s).wait_send()
    for copy in home_copies:
        copy(c).wait_send()
    home_copy.wait_send()
    sq_copy.wait_send()


def ring_local(
    n,
    tokens,
    expert_ids,
    gate_weights,
    norm_gain,
    expert_gate,
    expert_up,
    expert_down,
    shared_gate,
    shared_up,
    shared_down,
    out_gain,
):
    rows, width = tokens.shape
    ff = expert_gate.shape[2]
    sh = shared_gate.shape[1]
    cols = width // 2
    slots, turn = (n - 1) * PARTS, n // 2
    chunk = rows // (2 * PARTS)
    experts = 2 * n * expert_gate.shape[0]
    dma = pltpu.SemaphoreType.DMA
    vmem = pl.BlockSpec(memory_space=pltpu.VMEM)
    hbm = pl.BlockSpec(memory_space=pl.ANY)
    mixed, squares = pl.pallas_call(
        functools.partial(ring_kernel, n),
        out_shape=(
            jax.ShapeDtypeStruct((2 * rows, cols), BF16),
            jax.ShapeDtypeStruct((2 * rows, 128), F32),
        ),
        in_specs=[vmem] * 4 + [hbm] * 6,
        out_specs=(vmem, vmem),
        scratch_shapes=[
            pltpu.VMEM((2, rows, width), BF16),
            pltpu.VMEM((2, experts, rows), F32),
            pltpu.VMEM((slots, 2, 2, chunk, width), BF16),
            pltpu.VMEM((turn, 2, 2, experts, rows), F32),
            pltpu.VMEM((width, ff), BF16),
            pltpu.VMEM((width, ff), BF16),
            pltpu.VMEM((ff, cols), BF16),
            pltpu.VMEM((ff, cols), BF16),
            pltpu.VMEM((width, sh), BF16),
            pltpu.VMEM((width, sh), BF16),
            pltpu.VMEM((sh, cols), BF16),
            pltpu.VMEM((sh, cols), BF16),
            pltpu.VMEM((slots, 4 * chunk, cols), F32),
            pltpu.VMEM((slots, 4 * chunk, cols), BF16),
            pltpu.VMEM((slots, 4 * chunk, cols), BF16),
            pltpu.VMEM((2 * rows, cols), F32),
            pltpu.VMEM((2 * rows, cols), F32),
            pltpu.VMEM((2 * rows, cols), F32),
            pltpu.VMEM((slots, 2, 2 * chunk, cols), BF16),
            pltpu.VMEM((slots, 2, 2 * chunk, cols), BF16),
            pltpu.VMEM((2 * rows, 128), F32),
            pltpu.VMEM((2 * rows, 128), F32),
            dma((8,)),
            dma((slots, 2)),
            dma((slots, 2)),
            dma((turn, 2)),
            dma((turn, 2)),
            dma((slots, 2)),
            dma((slots, 2)),
            dma((turn, 2)),
            dma((turn, 2)),
            dma((2,)),
            dma((2,)),
            dma((slots,)),
            dma((slots,)),
            dma((1,)),
            dma((1,)),
            dma((slots, 2)),
            dma((slots, 2)),
            dma((1,)),
            dma((1,)),
        ],
        compiler_params=pltpu.CompilerParams(
            collective_id=0, has_side_effects=True, vmem_limit_bytes=60 * 1024 * 1024
        ),
    )(
        expert_ids.T,
        gate_weights.T,
        tokens,
        norm_gain.reshape(1, width),
        expert_gate,
        expert_up,
        expert_down,
        shared_gate,
        shared_up,
        shared_down,
    )
    scale = lax.rsqrt(squares[:, :1] / width + 1e-06)
    gain = lax.dynamic_slice(out_gain, (lax.axis_index("tp") * cols,), (cols,))
    return (mixed.astype(F32) * scale * gain).astype(BF16)


TOPK = 4


def expert_work(received, expert_gate, expert_up, expert_down):
    gate = jnp.einsum("slcd,ldf->slcf", received, expert_gate, preferred_element_type=jnp.float32)
    upper = jnp.einsum("slcd,ldf->slcf", received, expert_up, preferred_element_type=jnp.float32)
    hidden = (jax.nn.silu(gate) * upper).astype(jnp.bfloat16)
    return jnp.einsum(
        "slcf,lfd->slcd", hidden, expert_down, preferred_element_type=jnp.float32
    ).astype(jnp.bfloat16)


def local(
    tokens,
    expert_ids,
    gate_weights,
    norm_gain,
    expert_gate,
    expert_up,
    expert_down,
    shared_gate,
    shared_up,
    shared_down,
    out_gain,
):
    local_rows = tokens.shape[0]
    width = tokens.shape[1]
    ep_count = lax.axis_size("ep")
    tp_count = lax.axis_size("tp")
    device_count = ep_count * tp_count
    local_experts = expert_gate.shape[0]
    expert_count = device_count * local_experts
    capacity = 3 * local_rows * TOPK // (2 * expert_count)
    values = tokens.astype(jnp.float32)
    scale = lax.rsqrt(jnp.mean(values * values, axis=1, keepdims=True) + 1e-06)
    normed = (values * scale * norm_gain).astype(jnp.bfloat16)
    flat_ids = expert_ids.reshape(-1)
    one_hot = (flat_ids[:, None] == jnp.arange(expert_count, dtype=jnp.int32)[None, :]).astype(
        jnp.int32
    )
    earlier = jnp.cumsum(one_hot, axis=0) - one_hot
    slot_index = jnp.sum(earlier * one_hot, axis=1)
    target = flat_ids * capacity + slot_index
    copy_rows = normed[jnp.arange(local_rows * TOPK, dtype=jnp.int32) // TOPK]
    outgoing = jnp.zeros((expert_count * capacity, width), jnp.bfloat16).at[target].set(copy_rows)
    sending = outgoing.reshape(device_count, local_experts * capacity, width)
    received = lax.all_to_all(sending, ("ep", "tp"), split_axis=0, concat_axis=0, tiled=True)
    received = received.reshape(device_count, local_experts, capacity, width)
    results = expert_work(received, expert_gate, expert_up, expert_down)
    results = results.reshape(device_count, local_experts * capacity, width)
    returned = lax.all_to_all(results, ("ep", "tp"), split_axis=0, concat_axis=0, tiled=True)
    returned = returned.reshape(expert_count * capacity, width)
    picked = returned[target].astype(jnp.float32).reshape(local_rows, TOPK, width)
    routed = jnp.sum(picked * gate_weights[:, :, None], axis=1)
    piece = lax.all_gather(normed, "tp", axis=0, tiled=True)
    gate = jnp.dot(piece, shared_gate, preferred_element_type=jnp.float32)
    upper = jnp.dot(piece, shared_up, preferred_element_type=jnp.float32)
    shared_hidden = (jax.nn.silu(gate) * upper).astype(jnp.bfloat16)
    shared_out = lax.psum_scatter(
        jnp.dot(shared_hidden, shared_down, preferred_element_type=jnp.float32),
        "tp",
        scatter_dimension=0,
        tiled=True,
    )
    mixed = (routed + shared_out).astype(jnp.bfloat16)
    mixed_values = mixed.astype(jnp.float32)
    final_scale = lax.rsqrt(jnp.mean(mixed_values * mixed_values, axis=1, keepdims=True) + 1e-06)
    normalized = (mixed_values * final_scale * out_gain).astype(jnp.bfloat16)
    return lax.all_to_all(normalized, "tp", split_axis=1, concat_axis=0, tiled=True)


def solution(mesh):
    in_specs = (
        P(("grp", "ep", "tp"), None),
        P(("grp", "ep", "tp"), None),
        P(("grp", "ep", "tp"), None),
        P(),
        P(("ep", "tp"), None, None),
        P(("ep", "tp"), None, None),
        P(("ep", "tp"), None, None),
        P(None, "tp"),
        P(None, "tp"),
        P("tp", None),
        P(),
    )
    out_specs = P(("grp", "ep"), "tp")
    n, tp = mesh.shape["ep"], mesh.shape["tp"]

    def run(*args):
        tokens, expert_gate = args[0], args[4]
        rows = tokens.shape[0] // mesh.size
        experts = expert_gate.shape[0]
        dense = experts == n * tp and experts <= 8 * args[1].shape[1]
        dense = dense and tp == 2 and n % 2 == 0 and n >= 4 and rows == 128
        body = functools.partial(ring_local, n) if dense else local
        return jax.shard_map(
            body, mesh=mesh, in_specs=in_specs, out_specs=out_specs, check_vma=False
        )(*args)

    return run
```

```python
import functools

import jax
import jax.numpy as jnp
from jax import lax
from jax.experimental import pallas as pl
from jax.experimental.pallas import tpu as pltpu
from jax.sharding import PartitionSpec as P

MESH = pl.DeviceIdType.MESH
PARTS = 2
F32 = jnp.float32
BF16 = jnp.bfloat16


def ring_kernel(
    n,
    ids_ref,
    gates_ref,
    tok_hbm,
    gain_ref,
    out_gain_ref,
    eg_hbm,
    eu_hbm,
    ed_hbm,
    sg_hbm,
    su_hbm,
    sd_hbm,
    out_ref,
    tok,
    own_x,
    own_w,
    rx,
    wrx,
    wg,
    wu,
    wd_mine,
    wd_other,
    sg,
    su,
    sd_mine,
    sd_other,
    kept,
    psend,
    prx,
    home,
    home_send,
    home_rx,
    rs_send,
    rs_rx,
    sq_send,
    sq_rx,
    tok_sem,
    load_sem,
    ag_ssem,
    ag_rsem,
    w_ssem,
    w_rsem,
    pag_ssem,
    pag_rsem,
    pw_ssem,
    pw_rsem,
    ox_ssem,
    ox_rsem,
    p_ssem,
    p_rsem,
    h_ssem,
    h_rsem,
    rs_ssem,
    rs_rsem,
    sq_ssem,
    sq_rsem,
):
    per = 2 * PARTS
    slots = (n - 1) * PARTS
    rows, width = tok.shape
    chunk = rows // per
    cols = width // 2
    topk = ids_ref.shape[0]
    experts = own_w.shape[1]
    turn = n // 2
    ep = lax.axis_index("ep")
    c = lax.axis_index("tp")
    oc = 1 - c
    x = ep % 2
    z = ep // 2
    pos = z * (1 - x) + (n - 1 - z) * x

    def at(p):
        q = p // turn
        return 2 * p * (1 - q) + (2 * (n - 1 - p) + 1) * q

    toward = (at((pos + 1) % n), at((pos + n - 1) % n))
    mine = ep * 2 + c

    barrier = pltpu.get_barrier_semaphore()
    for e in toward:
        pl.semaphore_signal(barrier, inc=1, device_id={"ep": e, "tp": c}, device_id_type=MESH)
    pl.semaphore_signal(barrier, inc=1, device_id={"ep": ep, "tp": oc}, device_id_type=MESH)

    tok_loads = []
    for j, k in enumerate([k for s in range(PARTS) for k in (s, s + PARTS)]):
        part = pl.ds(k * chunk, chunk)
        tok_loads.append(pltpu.make_async_copy(tok_hbm.at[part], tok.at[part], tok_sem.at[j]))
        tok_loads[-1].start()

    lo, hi = pl.ds(pl.multiple_of(c * cols, cols), cols), pl.ds(pl.multiple_of(oc * cols, cols), cols)
    loads = [
        (eg_hbm.at[0], wg),
        (eu_hbm.at[0], wu),
        (ed_hbm.at[0, :, hi], wd_other),
        (ed_hbm.at[0, :, lo], wd_mine),
        (sg_hbm, sg),
        (su_hbm, su),
        (sd_hbm.at[:, hi], sd_other),
        (sd_hbm.at[:, lo], sd_mine),
    ]
    loads = [pltpu.make_async_copy(s, d, load_sem.at[i]) for i, (s, d) in enumerate(loads)]
    for load in loads:
        load.start()

    expert = lax.broadcasted_iota(jnp.int32, (experts, rows), 0)
    dense = jnp.zeros((experts, rows), F32)
    for k in range(topk):
        dense += jnp.where(ids_ref[k : k + 1, :] == expert, gates_ref[k : k + 1, :], 0.0)
    own_w[c] = dense

    def remote(src, dst, ssem, rsem, e, core):
        return pltpu.make_async_remote_copy(
            src_ref=src,
            dst_ref=dst,
            send_sem=ssem,
            recv_sem=rsem,
            device_id={"ep": e, "tp": core},
            device_id_type=MESH,
        )

    def ag(s, d, src):
        return remote(src, rx.at[s, d, c], ag_ssem.at[s, d], ag_rsem.at[s, d], toward[d], c)

    def agw(i, d, src):
        return remote(src, wrx.at[i, d, c], w_ssem.at[i, d], w_rsem.at[i, d], toward[d], c)

    def pag(s, d, core):
        return remote(
            rx.at[s, d, core], rx.at[s, d, core], pag_ssem.at[s, d], pag_rsem.at[s, d], ep, oc
        )

    def pagw(i, d, core):
        return remote(
            wrx.at[i, d, core], wrx.at[i, d, core], pw_ssem.at[i, d], pw_rsem.at[i, d], ep, oc
        )

    def place(s, d):
        return (s + d * PARTS) % per

    def own_chunk(s, d):
        return own_x.at[c, pl.ds(place(s, d) * chunk, chunk)]

    def normalise(k):
        part = pl.ds(k * chunk, chunk)
        values = tok[part, :].astype(F32)
        scale = lax.rsqrt(jnp.mean(values * values, axis=1, keepdims=True) + 1e-06)
        own_x[c, part, :] = (values * scale * gain_ref[...]).astype(BF16)

    for s in range(PARTS):
        for d in range(2):
            tok_loads[2 * s + d].wait()
            normalise(s + d * PARTS)
        if s == 0:
            pl.semaphore_wait(barrier, 3)
            for d in range(2):
                agw(0, d, own_w.at[c]).start()
        for d in range(2):
            ag(s, d, own_chunk(s, d)).start()
    for s in range(PARTS, per):
        for d in range(2):
            ag(s, d, own_chunk(s, d)).start()
    home_copies = (
        lambda core: remote(own_x.at[core], own_x.at[core], ox_ssem.at[0], ox_rsem.at[0], ep, oc),
        lambda core: remote(own_w.at[core], own_w.at[core], ox_ssem.at[1], ox_rsem.at[1], ep, oc),
    )
    for copy in home_copies:
        copy(c).start()

    def silu_mul(g, u):
        return (g / (1.0 + jnp.exp(-g)) * u).astype(BF16)

    def dot(a, b):
        return jnp.dot(a, b, preferred_element_type=F32)

    def column(row, offset, count):
        r = lax.broadcasted_iota(jnp.int32, (count, rows), 0) + offset
        q = lax.broadcasted_iota(jnp.int32, (count, rows), 1)
        return jnp.sum(jnp.where(r == q, row, 0.0), axis=1, keepdims=True)

    for load in loads:
        load.wait()
    for copy in home_copies:
        copy(oc).wait_recv()

    xs = own_x[...].reshape(2 * rows, width)
    hidden = silu_mul(dot(xs, wg[...]), dot(xs, wu[...]))
    shared = silu_mul(dot(xs, sg[...]), dot(xs, su[...]))
    weight = jnp.concatenate(
        [column(own_w[k, pl.ds(mine, 1), :], 0, rows) for k in range(2)], axis=0
    )
    home_send[...] = dot(hidden, wd_other[...]) * weight + dot(shared, sd_other[...])
    home[...] = dot(hidden, wd_mine[...]) * weight + dot(shared, sd_mine[...])
    home_copy = remote(home_send, home_rx, h_ssem.at[0], h_rsem.at[0], ep, oc)
    home_copy.start()

    def partner(s):
        return remote(psend.at[s], prx.at[s], p_ssem.at[s], p_rsem.at[s], ep, oc)

    def step(s, _):
        i = s // per
        first = s % per == 0
        for d in range(2):
            ag(s, d, rx.at[s, d, c]).wait_recv()

            @pl.when(s + per < slots)
            def _():
                ag(s + per, d, rx.at[s, d, c]).start()

            pag(s, d, c).start()

            @pl.when(first)
            def _():
                agw(i, d, wrx.at[i, d, c]).wait_recv()

                @pl.when(s + per < slots)
                def _():
                    agw(i + 1, d, wrx.at[i, d, c]).start()

                pagw(i, d, c).start()

        for d in range(2):
            pag(s, d, oc).wait_recv()

            @pl.when(first)
            def _():
                pagw(i, d, oc).wait_recv()

        weight = jnp.concatenate(
            [
                column(
                    wrx[i, d, k, pl.ds(mine, 1), :],
                    place(s, d) * chunk,
                    chunk,
                )
                for d in range(2)
                for k in range(2)
            ],
            axis=0,
        )
        xs = rx[s].reshape(4 * chunk, width)
        hidden = silu_mul(dot(xs, wg[...]), dot(xs, wu[...]))
        psend[s] = (dot(hidden, wd_other[...]) * weight).astype(BF16)
        kept[s] = dot(hidden, wd_mine[...]) * weight
        partner(s).start()
        return 0

    def back(s, d):
        return remote(
            rs_send.at[s, d], rs_rx.at[s, d], rs_ssem.at[s, d], rs_rsem.at[s, d], toward[1 - d], c
        )

    def give(s, further):
        partner(s).wait_recv()
        for d in range(2):
            part = pl.ds(d * 2 * chunk, 2 * chunk)
            total = kept[s, part, :] + prx[s, part, :].astype(F32)
            if further:
                back(s + per, d).wait_recv()
                total += rs_rx[s + per, d].astype(F32)
            rs_send[s, d] = total.astype(BF16)
            back(s, d).start()

    for s in range(slots - per, slots):
        lax.fori_loop(s if s > slots - per else 0, s + 1, step, 0)
        give(s, False)
    home_copy.wait_recv()
    home[...] += home_rx[...]
    order = [s for k in range(slots - 2 * per, -1, -per) for s in range(k, k + per)]
    for s in order + list(range(slots % per)):
        give(s, True)

    def squares(s):
        return remote(sq_send.at[s], sq_rx.at[s], sq_ssem.at[s], sq_rsem.at[s], ep, oc)

    def home_rows(s, d, k):
        return pl.ds(k * rows + place(s, d) * chunk, chunk)

    for s in [*range(PARTS, per), *range(PARTS)]:
        for d in range(2):
            back(s, d).wait_recv()
            for k in range(2):
                part = home_rows(s, d, k)
                total = home[part, :] + rs_rx[s, d, pl.ds(k * chunk, chunk), :].astype(F32)
                if s < PARTS:
                    total = total.astype(BF16).astype(F32)
                    sq = jnp.sum(total * total, axis=1, keepdims=True)
                    sq_send[s, pl.ds((2 * d + k) * chunk, chunk), :] = jnp.broadcast_to(
                        sq, (chunk, 128)
                    )
                home[part, :] = total
        if s < PARTS:
            squares(s).start()
    for s in range(PARTS):
        squares(s).wait_recv()
        final = lax.rsqrt((sq_send[s] + sq_rx[s])[:, :1] / width + 1e-06)
        for d in range(2):
            for k in range(2):
                part = home_rows(s, d, k)
                at_k = (2 * d + k) * chunk
                out_ref[part, :] = (
                    home[part, :] * final[at_k : at_k + chunk] * out_gain_ref[c]
                ).astype(BF16)

    for d in range(2):
        for s in range(slots):
            ag(s, d, rx.at[s, d, c]).wait_send()
            pag(s, d, c).wait_send()
            back(s, d).wait_send()
        for i in range(turn):
            agw(i, d, wrx.at[i, d, c]).wait_send()
            pagw(i, d, c).wait_send()
    for s in range(slots):
        partner(s).wait_send()
    for copy in home_copies:
        copy(c).wait_send()
    home_copy.wait_send()
    for s in range(PARTS):
        squares(s).wait_send()


def ring_local(
    n,
    tokens,
    expert_ids,
    gate_weights,
    norm_gain,
    expert_gate,
    expert_up,
    expert_down,
    shared_gate,
    shared_up,
    shared_down,
    out_gain,
):
    rows, width = tokens.shape
    ff = expert_gate.shape[2]
    sh = shared_gate.shape[1]
    cols = width // 2
    slots, turn = (n - 1) * PARTS, n // 2
    chunk = rows // (2 * PARTS)
    experts = 2 * n * expert_gate.shape[0]
    dma = pltpu.SemaphoreType.DMA
    vmem = pl.BlockSpec(memory_space=pltpu.VMEM)
    hbm = pl.BlockSpec(memory_space=pl.ANY)
    return pl.pallas_call(
        functools.partial(ring_kernel, n),
        out_shape=pltpu.VMEM((2 * rows, cols), BF16),
        in_specs=[vmem] * 2 + [hbm] + [vmem] * 2 + [hbm] * 6,
        out_specs=vmem,
        scratch_shapes=[
            pltpu.VMEM((rows, width), BF16),
            pltpu.VMEM((2, rows, width), BF16),
            pltpu.VMEM((2, experts, rows), F32),
            pltpu.VMEM((slots, 2, 2, chunk, width), BF16),
            pltpu.VMEM((turn, 2, 2, experts, rows), F32),
            pltpu.VMEM((width, ff), BF16),
            pltpu.VMEM((width, ff), BF16),
            pltpu.VMEM((ff, cols), BF16),
            pltpu.VMEM((ff, cols), BF16),
            pltpu.VMEM((width, sh), BF16),
            pltpu.VMEM((width, sh), BF16),
            pltpu.VMEM((sh, cols), BF16),
            pltpu.VMEM((sh, cols), BF16),
            pltpu.VMEM((slots, 4 * chunk, cols), F32),
            pltpu.VMEM((slots, 4 * chunk, cols), BF16),
            pltpu.VMEM((slots, 4 * chunk, cols), BF16),
            pltpu.VMEM((2 * rows, cols), F32),
            pltpu.VMEM((2 * rows, cols), F32),
            pltpu.VMEM((2 * rows, cols), F32),
            pltpu.VMEM((slots, 2, 2 * chunk, cols), BF16),
            pltpu.VMEM((slots, 2, 2 * chunk, cols), BF16),
            pltpu.VMEM((PARTS, 4 * chunk, 128), F32),
            pltpu.VMEM((PARTS, 4 * chunk, 128), F32),
            dma((2 * PARTS,)),
            dma((8,)),
            dma((slots, 2)),
            dma((slots, 2)),
            dma((turn, 2)),
            dma((turn, 2)),
            dma((slots, 2)),
            dma((slots, 2)),
            dma((turn, 2)),
            dma((turn, 2)),
            dma((2,)),
            dma((2,)),
            dma((slots,)),
            dma((slots,)),
            dma((1,)),
            dma((1,)),
            dma((slots, 2)),
            dma((slots, 2)),
            dma((PARTS,)),
            dma((PARTS,)),
        ],
        compiler_params=pltpu.CompilerParams(
            collective_id=0, has_side_effects=True, vmem_limit_bytes=60 * 1024 * 1024
        ),
    )(
        expert_ids.T,
        gate_weights.T,
        tokens,
        norm_gain.reshape(1, width),
        out_gain.reshape(2, 1, cols),
        expert_gate,
        expert_up,
        expert_down,
        shared_gate,
        shared_up,
        shared_down,
    )


TOPK = 4


def expert_work(received, expert_gate, expert_up, expert_down):
    gate = jnp.einsum("slcd,ldf->slcf", received, expert_gate, preferred_element_type=jnp.float32)
    upper = jnp.einsum("slcd,ldf->slcf", received, expert_up, preferred_element_type=jnp.float32)
    hidden = (jax.nn.silu(gate) * upper).astype(jnp.bfloat16)
    return jnp.einsum(
        "slcf,lfd->slcd", hidden, expert_down, preferred_element_type=jnp.float32
    ).astype(jnp.bfloat16)


def local(
    tokens,
    expert_ids,
    gate_weights,
    norm_gain,
    expert_gate,
    expert_up,
    expert_down,
    shared_gate,
    shared_up,
    shared_down,
    out_gain,
):
    local_rows = tokens.shape[0]
    width = tokens.shape[1]
    ep_count = lax.axis_size("ep")
    tp_count = lax.axis_size("tp")
    device_count = ep_count * tp_count
    local_experts = expert_gate.shape[0]
    expert_count = device_count * local_experts
    capacity = 3 * local_rows * TOPK // (2 * expert_count)
    values = tokens.astype(jnp.float32)
    scale = lax.rsqrt(jnp.mean(values * values, axis=1, keepdims=True) + 1e-06)
    normed = (values * scale * norm_gain).astype(jnp.bfloat16)
    flat_ids = expert_ids.reshape(-1)
    one_hot = (flat_ids[:, None] == jnp.arange(expert_count, dtype=jnp.int32)[None, :]).astype(
        jnp.int32
    )
    earlier = jnp.cumsum(one_hot, axis=0) - one_hot
    slot_index = jnp.sum(earlier * one_hot, axis=1)
    target = flat_ids * capacity + slot_index
    copy_rows = normed[jnp.arange(local_rows * TOPK, dtype=jnp.int32) // TOPK]
    outgoing = jnp.zeros((expert_count * capacity, width), jnp.bfloat16).at[target].set(copy_rows)
    sending = outgoing.reshape(device_count, local_experts * capacity, width)
    received = lax.all_to_all(sending, ("ep", "tp"), split_axis=0, concat_axis=0, tiled=True)
    received = received.reshape(device_count, local_experts, capacity, width)
    results = expert_work(received, expert_gate, expert_up, expert_down)
    results = results.reshape(device_count, local_experts * capacity, width)
    returned = lax.all_to_all(results, ("ep", "tp"), split_axis=0, concat_axis=0, tiled=True)
    returned = returned.reshape(expert_count * capacity, width)
    picked = returned[target].astype(jnp.float32).reshape(local_rows, TOPK, width)
    routed = jnp.sum(picked * gate_weights[:, :, None], axis=1)
    piece = lax.all_gather(normed, "tp", axis=0, tiled=True)
    gate = jnp.dot(piece, shared_gate, preferred_element_type=jnp.float32)
    upper = jnp.dot(piece, shared_up, preferred_element_type=jnp.float32)
    shared_hidden = (jax.nn.silu(gate) * upper).astype(jnp.bfloat16)
    shared_out = lax.psum_scatter(
        jnp.dot(shared_hidden, shared_down, preferred_element_type=jnp.float32),
        "tp",
        scatter_dimension=0,
        tiled=True,
    )
    mixed = (routed + shared_out).astype(jnp.bfloat16)
    mixed_values = mixed.astype(jnp.float32)
    final_scale = lax.rsqrt(jnp.mean(mixed_values * mixed_values, axis=1, keepdims=True) + 1e-06)
    normalized = (mixed_values * final_scale * out_gain).astype(jnp.bfloat16)
    return lax.all_to_all(normalized, "tp", split_axis=1, concat_axis=0, tiled=True)


def solution(mesh):
    in_specs = (
        P(("grp", "ep", "tp"), None),
        P(("grp", "ep", "tp"), None),
        P(("grp", "ep", "tp"), None),
        P(),
        P(("ep", "tp"), None, None),
        P(("ep", "tp"), None, None),
        P(("ep", "tp"), None, None),
        P(None, "tp"),
        P(None, "tp"),
        P("tp", None),
        P(),
    )
    out_specs = P(("grp", "ep"), "tp")
    n, tp = mesh.shape["ep"], mesh.shape["tp"]

    def run(*args):
        tokens, expert_gate = args[0], args[4]
        rows = tokens.shape[0] // mesh.size
        experts = expert_gate.shape[0]
        dense = experts == n * tp and experts <= 8 * args[1].shape[1]
        dense = dense and tp == 2 and n % 2 == 0 and n >= 4 and rows == 128
        body = functools.partial(ring_local, n) if dense else local
        return jax.shard_map(
            body, mesh=mesh, in_specs=in_specs, out_specs=out_specs, check_vma=False
        )(*args)

    return run
```

```python
import functools

import jax
import jax.numpy as jnp
from jax import lax
from jax.experimental import pallas as pl
from jax.experimental.pallas import tpu as pltpu
from jax.sharding import PartitionSpec as P

MESH = pl.DeviceIdType.MESH
PARTS = 2
F32 = jnp.float32
BF16 = jnp.bfloat16


def ring_kernel(
    n,
    ids_ref,
    gates_ref,
    tok_hbm,
    gain_ref,
    out_gain_ref,
    eg_hbm,
    eu_hbm,
    ed_hbm,
    sg_hbm,
    su_hbm,
    sd_hbm,
    out_ref,
    tok,
    own_x,
    own_w,
    rx,
    wrx,
    wg,
    wu,
    wd_mine,
    wd_other,
    sg,
    su,
    sd_mine,
    sd_other,
    kept,
    psend,
    prx,
    home,
    home_send,
    home_rx,
    rs_send,
    rs_rx,
    sq_send,
    sq_rx,
    tok_sem,
    load_sem,
    ag_ssem,
    ag_rsem,
    w_ssem,
    w_rsem,
    pag_ssem,
    pag_rsem,
    pw_ssem,
    pw_rsem,
    ox_ssem,
    ox_rsem,
    p_ssem,
    p_rsem,
    h_ssem,
    h_rsem,
    rs_ssem,
    rs_rsem,
    sq_ssem,
    sq_rsem,
):
    per = 2 * PARTS
    slots = (n - 1) * PARTS
    rows, width = tok.shape
    chunk = rows // per
    cols = width // 2
    topk = ids_ref.shape[0]
    experts = own_w.shape[1]
    turn = n // 2
    ep = lax.axis_index("ep")
    c = lax.axis_index("tp")
    oc = 1 - c
    x = ep % 2
    z = ep // 2
    pos = z * (1 - x) + (n - 1 - z) * x

    def at(p):
        q = p // turn
        return 2 * p * (1 - q) + (2 * (n - 1 - p) + 1) * q

    toward = (at((pos + 1) % n), at((pos + n - 1) % n))
    mine = ep * 2 + c

    barrier = pltpu.get_barrier_semaphore()
    for e in toward:
        pl.semaphore_signal(barrier, inc=1, device_id={"ep": e, "tp": c}, device_id_type=MESH)
    pl.semaphore_signal(barrier, inc=1, device_id={"ep": ep, "tp": oc}, device_id_type=MESH)

    tok_loads = []
    for j, k in enumerate([k for s in range(PARTS) for k in (s, s + PARTS)]):
        part = pl.ds(k * chunk, chunk)
        tok_loads.append(pltpu.make_async_copy(tok_hbm.at[part], tok.at[part], tok_sem.at[j]))
        tok_loads[-1].start()

    lo, hi = pl.ds(pl.multiple_of(c * cols, cols), cols), pl.ds(pl.multiple_of(oc * cols, cols), cols)
    loads = [
        (eg_hbm.at[0], wg),
        (eu_hbm.at[0], wu),
        (ed_hbm.at[0, :, hi], wd_other),
        (ed_hbm.at[0, :, lo], wd_mine),
        (sg_hbm, sg),
        (su_hbm, su),
        (sd_hbm.at[:, hi], sd_other),
        (sd_hbm.at[:, lo], sd_mine),
    ]
    loads = [pltpu.make_async_copy(s, d, load_sem.at[i]) for i, (s, d) in enumerate(loads)]
    for load in loads:
        load.start()

    expert = lax.broadcasted_iota(jnp.int32, (experts, rows), 0)
    dense = jnp.zeros((experts, rows), F32)
    for k in range(topk):
        dense += jnp.where(ids_ref[k : k + 1, :] == expert, gates_ref[k : k + 1, :], 0.0)
    own_w[c] = dense

    def remote(src, dst, ssem, rsem, e, core):
        return pltpu.make_async_remote_copy(
            src_ref=src,
            dst_ref=dst,
            send_sem=ssem,
            recv_sem=rsem,
            device_id={"ep": e, "tp": core},
            device_id_type=MESH,
        )

    def ag(s, d, src):
        return remote(src, rx.at[s, d, c], ag_ssem.at[s, d], ag_rsem.at[s, d], toward[d], c)

    def agw(i, d, src):
        return remote(src, wrx.at[i, d, c], w_ssem.at[i, d], w_rsem.at[i, d], toward[d], c)

    def pag(s, d, core):
        return remote(
            rx.at[s, d, core], rx.at[s, d, core], pag_ssem.at[s, d], pag_rsem.at[s, d], ep, oc
        )

    def pagw(i, d, core):
        return remote(
            wrx.at[i, d, core], wrx.at[i, d, core], pw_ssem.at[i, d], pw_rsem.at[i, d], ep, oc
        )

    def place(s, d):
        return (s + d * PARTS) % per

    def own_chunk(s, d):
        return own_x.at[c, pl.ds(place(s, d) * chunk, chunk)]

    def normalise(k):
        part = pl.ds(k * chunk, chunk)
        values = tok[part, :].astype(F32)
        scale = lax.rsqrt(jnp.mean(values * values, axis=1, keepdims=True) + 1e-06)
        own_x[c, part, :] = (values * scale * gain_ref[...]).astype(BF16)

    for s in range(PARTS):
        for d in range(2):
            tok_loads[2 * s + d].wait()
            normalise(s + d * PARTS)
        if s == 0:
            pl.semaphore_wait(barrier, 3)
            for d in range(2):
                agw(0, d, own_w.at[c]).start()
        for d in range(2):
            ag(s, d, own_chunk(s, d)).start()
    for s in range(PARTS, per):
        for d in range(2):
            ag(s, d, own_chunk(s, d)).start()
    home_copies = (
        lambda core: remote(own_x.at[core], own_x.at[core], ox_ssem.at[0], ox_rsem.at[0], ep, oc),
        lambda core: remote(own_w.at[core], own_w.at[core], ox_ssem.at[1], ox_rsem.at[1], ep, oc),
    )
    for copy in home_copies:
        copy(c).start()

    def relay(s):
        i = s // per
        first = s % per == 0
        for d in range(2):
            ag(s, d, rx.at[s, d, c]).wait_recv()

            @pl.when(s + per < slots)
            def _():
                ag(s + per, d, rx.at[s, d, c]).start()

            pag(s, d, c).start()

            @pl.when(first)
            def _():
                agw(i, d, wrx.at[i, d, c]).wait_recv()

                @pl.when(s + per < slots)
                def _():
                    agw(i + 1, d, wrx.at[i, d, c]).start()

                pagw(i, d, c).start()

    relay(0)

    def silu_mul(g, u):
        return (g / (1.0 + jnp.exp(-g)) * u).astype(BF16)

    def dot(a, b):
        return jnp.dot(a, b, preferred_element_type=F32)

    def column(row, offset, count):
        r = lax.broadcasted_iota(jnp.int32, (count, rows), 0) + offset
        q = lax.broadcasted_iota(jnp.int32, (count, rows), 1)
        return jnp.sum(jnp.where(r == q, row, 0.0), axis=1, keepdims=True)

    for load in loads:
        load.wait()
    for copy in home_copies:
        copy(oc).wait_recv()

    xs = own_x[...].reshape(2 * rows, width)
    hidden = silu_mul(dot(xs, wg[...]), dot(xs, wu[...]))
    shared = silu_mul(dot(xs, sg[...]), dot(xs, su[...]))
    weight = jnp.concatenate(
        [column(own_w[k, pl.ds(mine, 1), :], 0, rows) for k in range(2)], axis=0
    )
    home_send[...] = dot(hidden, wd_other[...]) * weight + dot(shared, sd_other[...])
    home[...] = dot(hidden, wd_mine[...]) * weight + dot(shared, sd_mine[...])
    home_copy = remote(home_send, home_rx, h_ssem.at[0], h_rsem.at[0], ep, oc)
    home_copy.start()

    def partner(s):
        return remote(psend.at[s], prx.at[s], p_ssem.at[s], p_rsem.at[s], ep, oc)

    def work(s):
        i = s // per
        first = s % per == 0
        for d in range(2):
            pag(s, d, oc).wait_recv()

            @pl.when(first)
            def _():
                pagw(i, d, oc).wait_recv()

        weight = jnp.concatenate(
            [
                column(
                    wrx[i, d, k, pl.ds(mine, 1), :],
                    place(s, d) * chunk,
                    chunk,
                )
                for d in range(2)
                for k in range(2)
            ],
            axis=0,
        )
        xs = rx[s].reshape(4 * chunk, width)
        hidden = silu_mul(dot(xs, wg[...]), dot(xs, wu[...]))
        psend[s] = (dot(hidden, wd_other[...]) * weight).astype(BF16)
        kept[s] = dot(hidden, wd_mine[...]) * weight
        partner(s).start()

    def back(s, d):
        return remote(
            rs_send.at[s, d], rs_rx.at[s, d], rs_ssem.at[s, d], rs_rsem.at[s, d], toward[1 - d], c
        )

    def give(s, further):
        partner(s).wait_recv()
        for d in range(2):
            part = pl.ds(d * 2 * chunk, 2 * chunk)
            total = kept[s, part, :] + prx[s, part, :].astype(F32)
            if further:
                back(s + per, d).wait_recv()
                total += rs_rx[s + per, d].astype(F32)
            rs_send[s, d] = total.astype(BF16)
            back(s, d).start()

    def step(s, _):
        relay(s + 1)
        work(s)
        return 0

    lax.fori_loop(0, slots - per, step, 0)
    for s in range(slots - per, slots):
        if s + 1 < slots:
            lax.fori_loop(s, s + 1, step, 0)
        else:
            work(s)
        if s > slots - per:
            give(s - 1, False)
    give(slots - 1, False)
    home_copy.wait_recv()
    home[...] += home_rx[...]
    order = [s for k in range(slots - 2 * per, -1, -per) for s in range(k, k + per)]
    for s in order + list(range(slots % per)):
        give(s, True)

    def squares(s):
        return remote(sq_send.at[s], sq_rx.at[s], sq_ssem.at[s], sq_rsem.at[s], ep, oc)

    def home_rows(s, d, k):
        return pl.ds(k * rows + place(s, d) * chunk, chunk)

    for s in [*range(PARTS, per), *range(PARTS)]:
        for d in range(2):
            back(s, d).wait_recv()
            for k in range(2):
                part = home_rows(s, d, k)
                total = home[part, :] + rs_rx[s, d, pl.ds(k * chunk, chunk), :].astype(F32)
                if s < PARTS:
                    total = total.astype(BF16).astype(F32)
                    sq = jnp.sum(total * total, axis=1, keepdims=True)
                    sq_send[s, pl.ds((2 * d + k) * chunk, chunk), :] = jnp.broadcast_to(
                        sq, (chunk, 128)
                    )
                home[part, :] = total
        if s < PARTS:
            squares(s).start()
    for s in range(PARTS):
        squares(s).wait_recv()
        final = lax.rsqrt((sq_send[s] + sq_rx[s])[:, :1] / width + 1e-06)
        for d in range(2):
            for k in range(2):
                part = home_rows(s, d, k)
                at_k = (2 * d + k) * chunk
                out_ref[part, :] = (
                    home[part, :] * final[at_k : at_k + chunk] * out_gain_ref[c]
                ).astype(BF16)

    for d in range(2):
        for s in range(slots):
            ag(s, d, rx.at[s, d, c]).wait_send()
            pag(s, d, c).wait_send()
            back(s, d).wait_send()
        for i in range(turn):
            agw(i, d, wrx.at[i, d, c]).wait_send()
            pagw(i, d, c).wait_send()
    for s in range(slots):
        partner(s).wait_send()
    for copy in home_copies:
        copy(c).wait_send()
    home_copy.wait_send()
    for s in range(PARTS):
        squares(s).wait_send()


def ring_local(
    n,
    tokens,
    expert_ids,
    gate_weights,
    norm_gain,
    expert_gate,
    expert_up,
    expert_down,
    shared_gate,
    shared_up,
    shared_down,
    out_gain,
):
    rows, width = tokens.shape
    ff = expert_gate.shape[2]
    sh = shared_gate.shape[1]
    cols = width // 2
    slots, turn = (n - 1) * PARTS, n // 2
    chunk = rows // (2 * PARTS)
    experts = 2 * n * expert_gate.shape[0]
    dma = pltpu.SemaphoreType.DMA
    vmem = pl.BlockSpec(memory_space=pltpu.VMEM)
    hbm = pl.BlockSpec(memory_space=pl.ANY)
    return pl.pallas_call(
        functools.partial(ring_kernel, n),
        out_shape=pltpu.VMEM((2 * rows, cols), BF16),
        in_specs=[vmem] * 2 + [hbm] + [vmem] * 2 + [hbm] * 6,
        out_specs=vmem,
        scratch_shapes=[
            pltpu.VMEM((rows, width), BF16),
            pltpu.VMEM((2, rows, width), BF16),
            pltpu.VMEM((2, experts, rows), F32),
            pltpu.VMEM((slots, 2, 2, chunk, width), BF16),
            pltpu.VMEM((turn, 2, 2, experts, rows), F32),
            pltpu.VMEM((width, ff), BF16),
            pltpu.VMEM((width, ff), BF16),
            pltpu.VMEM((ff, cols), BF16),
            pltpu.VMEM((ff, cols), BF16),
            pltpu.VMEM((width, sh), BF16),
            pltpu.VMEM((width, sh), BF16),
            pltpu.VMEM((sh, cols), BF16),
            pltpu.VMEM((sh, cols), BF16),
            pltpu.VMEM((slots, 4 * chunk, cols), F32),
            pltpu.VMEM((slots, 4 * chunk, cols), BF16),
            pltpu.VMEM((slots, 4 * chunk, cols), BF16),
            pltpu.VMEM((2 * rows, cols), F32),
            pltpu.VMEM((2 * rows, cols), F32),
            pltpu.VMEM((2 * rows, cols), F32),
            pltpu.VMEM((slots, 2, 2 * chunk, cols), BF16),
            pltpu.VMEM((slots, 2, 2 * chunk, cols), BF16),
            pltpu.VMEM((PARTS, 4 * chunk, 128), F32),
            pltpu.VMEM((PARTS, 4 * chunk, 128), F32),
            dma((2 * PARTS,)),
            dma((8,)),
            dma((slots, 2)),
            dma((slots, 2)),
            dma((turn, 2)),
            dma((turn, 2)),
            dma((slots, 2)),
            dma((slots, 2)),
            dma((turn, 2)),
            dma((turn, 2)),
            dma((2,)),
            dma((2,)),
            dma((slots,)),
            dma((slots,)),
            dma((1,)),
            dma((1,)),
            dma((slots, 2)),
            dma((slots, 2)),
            dma((PARTS,)),
            dma((PARTS,)),
        ],
        compiler_params=pltpu.CompilerParams(
            collective_id=0, has_side_effects=True, vmem_limit_bytes=60 * 1024 * 1024
        ),
    )(
        expert_ids.T,
        gate_weights.T,
        tokens,
        norm_gain.reshape(1, width),
        out_gain.reshape(2, 1, cols),
        expert_gate,
        expert_up,
        expert_down,
        shared_gate,
        shared_up,
        shared_down,
    )


TOPK = 4


def expert_work(received, expert_gate, expert_up, expert_down):
    gate = jnp.einsum("slcd,ldf->slcf", received, expert_gate, preferred_element_type=jnp.float32)
    upper = jnp.einsum("slcd,ldf->slcf", received, expert_up, preferred_element_type=jnp.float32)
    hidden = (jax.nn.silu(gate) * upper).astype(jnp.bfloat16)
    return jnp.einsum(
        "slcf,lfd->slcd", hidden, expert_down, preferred_element_type=jnp.float32
    ).astype(jnp.bfloat16)


def local(
    tokens,
    expert_ids,
    gate_weights,
    norm_gain,
    expert_gate,
    expert_up,
    expert_down,
    shared_gate,
    shared_up,
    shared_down,
    out_gain,
):
    local_rows = tokens.shape[0]
    width = tokens.shape[1]
    ep_count = lax.axis_size("ep")
    tp_count = lax.axis_size("tp")
    device_count = ep_count * tp_count
    local_experts = expert_gate.shape[0]
    expert_count = device_count * local_experts
    capacity = 3 * local_rows * TOPK // (2 * expert_count)
    values = tokens.astype(jnp.float32)
    scale = lax.rsqrt(jnp.mean(values * values, axis=1, keepdims=True) + 1e-06)
    normed = (values * scale * norm_gain).astype(jnp.bfloat16)
    flat_ids = expert_ids.reshape(-1)
    one_hot = (flat_ids[:, None] == jnp.arange(expert_count, dtype=jnp.int32)[None, :]).astype(
        jnp.int32
    )
    earlier = jnp.cumsum(one_hot, axis=0) - one_hot
    slot_index = jnp.sum(earlier * one_hot, axis=1)
    target = flat_ids * capacity + slot_index
    copy_rows = normed[jnp.arange(local_rows * TOPK, dtype=jnp.int32) // TOPK]
    outgoing = jnp.zeros((expert_count * capacity, width), jnp.bfloat16).at[target].set(copy_rows)
    sending = outgoing.reshape(device_count, local_experts * capacity, width)
    received = lax.all_to_all(sending, ("ep", "tp"), split_axis=0, concat_axis=0, tiled=True)
    received = received.reshape(device_count, local_experts, capacity, width)
    results = expert_work(received, expert_gate, expert_up, expert_down)
    results = results.reshape(device_count, local_experts * capacity, width)
    returned = lax.all_to_all(results, ("ep", "tp"), split_axis=0, concat_axis=0, tiled=True)
    returned = returned.reshape(expert_count * capacity, width)
    picked = returned[target].astype(jnp.float32).reshape(local_rows, TOPK, width)
    routed = jnp.sum(picked * gate_weights[:, :, None], axis=1)
    piece = lax.all_gather(normed, "tp", axis=0, tiled=True)
    gate = jnp.dot(piece, shared_gate, preferred_element_type=jnp.float32)
    upper = jnp.dot(piece, shared_up, preferred_element_type=jnp.float32)
    shared_hidden = (jax.nn.silu(gate) * upper).astype(jnp.bfloat16)
    shared_out = lax.psum_scatter(
        jnp.dot(shared_hidden, shared_down, preferred_element_type=jnp.float32),
        "tp",
        scatter_dimension=0,
        tiled=True,
    )
    mixed = (routed + shared_out).astype(jnp.bfloat16)
    mixed_values = mixed.astype(jnp.float32)
    final_scale = lax.rsqrt(jnp.mean(mixed_values * mixed_values, axis=1, keepdims=True) + 1e-06)
    normalized = (mixed_values * final_scale * out_gain).astype(jnp.bfloat16)
    return lax.all_to_all(normalized, "tp", split_axis=1, concat_axis=0, tiled=True)


def solution(mesh):
    in_specs = (
        P(("grp", "ep", "tp"), None),
        P(("grp", "ep", "tp"), None),
        P(("grp", "ep", "tp"), None),
        P(),
        P(("ep", "tp"), None, None),
        P(("ep", "tp"), None, None),
        P(("ep", "tp"), None, None),
        P(None, "tp"),
        P(None, "tp"),
        P("tp", None),
        P(),
    )
    out_specs = P(("grp", "ep"), "tp")
    n, tp = mesh.shape["ep"], mesh.shape["tp"]

    def run(*args):
        tokens, expert_gate = args[0], args[4]
        rows = tokens.shape[0] // mesh.size
        experts = expert_gate.shape[0]
        dense = experts == n * tp and experts <= 8 * args[1].shape[1]
        dense = dense and tp == 2 and n % 2 == 0 and n >= 4 and rows == 128
        body = functools.partial(ring_local, n) if dense else local
        return jax.shard_map(
            body, mesh=mesh, in_specs=in_specs, out_specs=out_specs, check_vma=False
        )(*args)

    return run
```
